128 devices in a mesh: sp: 64 (over z, y, x), tp: 2 (over core).
Axes of the slice: x: 4, y: 4, z: 4, core: 2. Of those that a mesh axis runs over, the one named last changes fastest.
Arguments:
- residual: bfloat16 [16384, 2048], P(('sp', 'tp')), may hold values from -6 to 6
- queries: bfloat16 [16384, 1024], P('sp', 'tp'), may hold values from -6 to 6
- keys: bfloat16 [16384, 1024], P('sp', 'tp'), may hold values from -6 to 6
- values: bfloat16 [16384, 2048], P('sp', 'tp'), may hold values from -6 to 6
- out_gate: bfloat16 [16384, 2048], P('sp', 'tp'), may hold values from -6 to 6
- in_gate: float32 [2, 16384, 8], P(None, 'sp', 'tp'), may hold values from -6 to 140, as said below
- forget_gate: float32 [2, 16384, 8], P(None, 'sp', 'tp'), may hold values from 0 to 20
- head_gain: float32 [2048], P('tp'), may hold values from 0.1 to 1.9
- w_out: bfloat16 [2048, 2048], P('tp'), may hold values from -0.125 to 0.125
- norm_gain: float32 [2048], replicated, may hold values from 0.1 to 1.9
- shared_gate: bfloat16 [2048, 512], replicated, may hold values from -0.125 to 0.125
- shared_up: bfloat16 [2048, 512], replicated, may hold values from -0.125 to 0.125
- shared_down: bfloat16 [512, 2048], replicated, may hold values from -0.25 to 0.25
- w_gate: bfloat16 [128, 2048, 512], P(('sp', 'tp')), may hold values from -0.125 to 0.125
- w_up: bfloat16 [128, 2048, 512], P(('sp', 'tp')), may hold values from -0.125 to 0.125
- w_down: bfloat16 [128, 512, 2048], P(('sp', 'tp')), may hold values from -0.25 to 0.25
- routes: int32 [16384, 4], P(('sp', 'tp')), may hold values from 0 to 127, all different within a row; in each aligned block of 128 rows (0 to 127, 128 to 255, ...) at most 8 rows name the same one
- route_weight: float32 [16384, 4], P(('sp', 'tp')), may hold values from 0.3 to 1.5
Outputs:
- layer_out: bfloat16 [16384, 2048], P(('sp', 'tp'))
The draws below stay inside these ranges and needn't reach their ends.
Inputs may be any that keep to these rules, and one draw needn't show every extreme that they name: `in_gate`: log input gates mostly of order one. `routes`: each row names 4 different experts. Among the rows of one device (aligned blocks of 128 rows) no expert is named more than 8 times, a bound that some block reaches.
All inputs are finite; a program needn't handle non-finite values.
Results may differ from the reference program's by a relative error of at most 0.017.
Values may be sent and summed in bfloat16 or wider, within the bound.
A program may use at most 128 MiB of HBM per device.

```python
import math
import jax
import jax.numpy as jnp
import numpy as np
from jax import lax

D = 2048
MEMORY_SPLITS = 8
DQK = 128
DV = 256
EXPERT_FF = 512
SHARED_FF = 512
TOP_K = 4
TOK_DEV = 256
TOK_HALF = 128
TOKENS = 16384
EXPERTS = 128
CAP = 8


def draw_in_gate(key, part):
    lookup_series = jax.random.split(key, 1)
    shape = (2, TOKENS, MEMORY_SPLITS)
    switch_levels = jnp.clip(jax.random.normal(lookup_series[0], shape, jnp.float32), -6.0, 6.0)
    return switch_levels.astype(jnp.float32)


def draw_forget_gate(key, part):
    lookup_series = jax.random.split(key, 5)
    shape = (2, TOKENS, MEMORY_SPLITS)
    fast_heads = jax.random.bernoulli(lookup_series[0], 0.5, (2, 1, MEMORY_SPLITS))
    noise = jnp.clip(jax.random.normal(lookup_series[2], shape, jnp.float32) * 0.8, -2.4, 2.4)
    level = jnp.where(fast_heads, math.log(40.0), math.log(TOKENS) + 1.1)
    block_count = TOKENS // TOK_DEV
    shift = jnp.repeat(jax.random.uniform(lookup_series[1], (2, block_count, MEMORY_SPLITS), jnp.float32, -0.7, 0.7), TOK_DEV, axis=1)
    switch_levels = level + shift + noise
    bucket_indices = jax.random.randint(lookup_series[3], (2, 3), 0, TOKENS)
    packet_bundles = jax.random.uniform(lookup_series[4], (2, 3, MEMORY_SPLITS), jnp.float32, 0.0, 1.4)
    sweep_heading = jnp.arange(2)[:, None]
    switch_levels = switch_levels.at[sweep_heading, bucket_indices].set(packet_bundles)
    return jnp.clip(switch_levels, 0.0, 20.0).astype(jnp.float32)


def block_scale(key, extent, cuts, least, top_value):
    def one(axis_at, shards_of):
        steps = jax.random.uniform(jax.random.fold_in(jax.random.fold_in(key, 6), axis_at), (shards_of,), jnp.float32, least / len(cuts), top_value / len(cuts))
        return jnp.repeat(jnp.exp(steps), extent[axis_at] // shards_of).reshape((-1,) + (1,) * (len(extent) - axis_at - 1))

    factor_of = one(*cuts[0])
    for cut in cuts[1:]:
        factor_of = factor_of * one(*cut)
    return factor_of


def routed_block(rng, own, number, rows, count, top, bound, skew):
    order = jax.random.permutation(rng, count)
    packed, usual = shares(count, rows * top, bound, skew, True), shares(count, rows * top, bound, skew, False)
    places = jnp.arange(count)

    def named(tallies, offset_by):
        used = int((tallies > 0).sum())
        fixed = max(1, used // 4)
        shifted = fixed + (places - fixed + offset_by * (used - fixed)) % max(1, count - fixed)
        return jnp.zeros((count,), jnp.int32).at[order[jnp.where(places < fixed, places, shifted)]].set(jnp.asarray(tallies, jnp.int32))

    tallies = jnp.where(number % 4 == 0, named(packed, number // 4), named(usual, number - number // 4 - 1))
    mixed = jax.random.permutation(jax.random.fold_in(own, 3), count)
    donor, receiver = mixed[0:count // 2 * 2:2], mixed[1:count // 2 * 2:2]
    slack = jnp.minimum(tallies[donor] - 1, bound - tallies[receiver]) // 2
    slack = jnp.where((donor == order[0]) | (receiver == order[0]) | (tallies[receiver] == 0), 0, jnp.maximum(slack, 0))
    shifted = jax.random.randint(jax.random.fold_in(own, 4), (count // 2,), 0, 1 << 20) % (slack + 1)
    tallies = tallies.at[donor].add(-shifted).at[receiver].add(shifted)
    items = jnp.searchsorted(jnp.cumsum(tallies), jnp.arange(rows * top), side="right").astype(jnp.int32)
    table = items.reshape(top, rows).T
    table = table[jax.random.permutation(jax.random.fold_in(own, 1), rows)]
    offset_by = jax.random.randint(jax.random.fold_in(own, 2), (rows, 1), 0, top)
    return jnp.take_along_axis(table, (jnp.arange(top)[None, :] + offset_by) % top, axis=1)


def shares(amount, total, most, skew, full):
    loads = [(1 << 20) // math.isqrt(standing ** skew) + 1 for standing in range(1, amount + 1)]
    largest = most if full else min(most, max(-(-total // amount), total * loads[0] // sum(loads)))
    least = 1 if total - largest >= amount - 1 else 0
    holding, surplus = [largest] + [least] * (amount - 1), total - largest - least * (amount - 1)
    while surplus > 0:
        free = [i for i in range(1, amount) if holding[i] < largest] or [i for i in range(1, amount) if holding[i] < most]
        pool, budget = sum([loads[i] for i in free]), surplus
        for i in free:
            extra = min(most - holding[i], max(1, budget * loads[i] // pool), surplus)
            holding[i] = holding[i] + extra
            surplus = surplus - extra
    return np.array(holding)


def centred(own_key, shape, scale, bound, cuts=(), held_as=jnp.bfloat16):
    loudness = block_scale(own_key, shape, cuts, -0.22, 0.18) if cuts else 1.0
    array = jax.random.normal(own_key, shape, jnp.float32) * scale * loudness
    return jnp.minimum(jnp.maximum(array, -bound), bound).astype(held_as)


def setup_inputs(seed: int = 0) -> dict:
    key_of = jax.random.split(jax.random.key(seed), 19)
    residual = centred(key_of[0], (TOKENS, D), 1.0, 6.0, ((0, 128),))
    queries = centred(key_of[1], (TOKENS, MEMORY_SPLITS * DQK), 1.0, 6.0, ((0, 64), (1, 2)))
    keys = centred(key_of[2], (TOKENS, MEMORY_SPLITS * DQK), 1.0, 6.0, ((0, 64), (1, 2)))
    values = centred(key_of[3], (TOKENS, MEMORY_SPLITS * DV), 1.0, 6.0, ((0, 64), (1, 2)))
    out_gate = centred(key_of[4], (TOKENS, MEMORY_SPLITS * DV), 1.5, 6.0, ((0, 64), (1, 2)))
    in_gate = draw_in_gate(jax.random.fold_in(key_of[18], 71), 0)
    forget_gate = draw_forget_gate(jax.random.fold_in(key_of[18], 71), 0)
    head_gain = jnp.clip(1.0 + 0.18 * jax.random.normal(key_of[7], (MEMORY_SPLITS * DV,), jnp.float32), 0.1, 1.9)
    w_out = centred(key_of[8], (MEMORY_SPLITS * DV, D), (MEMORY_SPLITS * DV) ** -0.5, 0.125, ((0, 2),))
    norm_gain = jnp.clip(1.0 + 0.18 * jax.random.normal(key_of[9], (D,), jnp.float32), 0.1, 1.9)
    shared_gate = centred(key_of[10], (D, SHARED_FF), D ** -0.5, 0.125)
    shared_up = centred(key_of[11], (D, SHARED_FF), D ** -0.5, 0.125)
    shared_down = centred(key_of[12], (SHARED_FF, D), SHARED_FF ** -0.5, 0.25)
    w_gate = centred(key_of[13], (EXPERTS, D, EXPERT_FF), D ** -0.5, 0.125, ((0, 128),))
    w_up = centred(key_of[14], (EXPERTS, D, EXPERT_FF), D ** -0.5, 0.125, ((0, 128),))
    w_down = centred(key_of[15], (EXPERTS, EXPERT_FF, D), EXPERT_FF ** -0.5, 0.25, ((0, 128),))
    routes_keys = jax.random.split(jax.random.fold_in(key_of[16], 1), TOKENS // TOK_HALF)
    routes_turns = jax.random.permutation(jax.random.fold_in(key_of[16], 3), TOKENS // TOK_HALF)
    routes = jax.vmap(lambda own, number: routed_block(jax.random.fold_in(key_of[16], 2), own, number, TOK_HALF, EXPERTS, TOP_K, CAP, 2))(routes_keys, routes_turns).reshape((TOKENS, TOP_K))
    route_weight = jnp.clip(jnp.exp(math.log(1.5) - 1.60943787 * jax.random.uniform(key_of[17], (TOKENS, TOP_K), jnp.float32) ** block_scale(key_of[17], (TOKENS, TOP_K), ((0, 128),), -0.2, 0.2)), 0.3, 1.5)
    return {"residual": residual, "queries": queries, "keys": keys, "values": values, "out_gate": out_gate, "in_gate": in_gate, "forget_gate": forget_gate, "head_gain": head_gain, "w_out": w_out, "norm_gain": norm_gain, "shared_gate": shared_gate, "shared_up": shared_up, "shared_down": shared_down, "w_gate": w_gate, "w_up": w_up, "w_down": w_down, "routes": routes, "route_weight": route_weight}


epsilon = 1e-06
max_floor = -1e+30
block_rows = 128

def direction_pass(query_heads, key_heads, value_heads, gate_input, log_forget, block_len):
    seq_len, head_count, key_dim = key_heads.shape
    value_dim = value_heads.shape[2]
    block_count = seq_len // block_len
    key_scale = 1.0 / math.sqrt(key_dim)
    pieces_all = (query_heads.reshape(block_count, block_len, head_count, key_dim), key_heads.reshape(block_count, block_len, head_count, key_dim), value_heads.reshape(block_count, block_len, head_count, value_dim), gate_input.reshape(block_count, block_len, head_count), log_forget.reshape(block_count, block_len, head_count))
    lower = jnp.tril(jnp.ones((block_len, block_len), dtype=bool))

    def block_step(carry, pieces):
        state_matrix, state_norm, state_max = carry
        block_query, block_key, block_value, block_in, block_forget = pieces
        running = jnp.cumsum(block_forget, axis=0)
        block_decay = running[-1]
        log_weight = block_decay[None, :] - running + block_in
        block_max = lax.optimization_barrier(jnp.max(log_weight, axis=0))
        scaled = jnp.exp(log_weight - block_max[None, :]) * key_scale
        weighted_low = lax.optimization_barrier((block_key.astype(jnp.float32) * scaled[:, :, None]).astype(jnp.bfloat16))
        weighted_keys = weighted_low.astype(jnp.float32)
        value_wide = block_value.astype(jnp.float32)
        query_wide = block_query.astype(jnp.float32)
        block_matrix = jnp.einsum('thd,the->hde', weighted_keys, value_wide)
        block_norm = lax.optimization_barrier(jnp.sum(weighted_keys, axis=0))
        running_heads = running.T
        pair_log = running_heads[:, :, None] - running_heads[:, None, :] + block_in.T[:, None, :]
        pair_log = jnp.where(lower[None], pair_log, -jnp.inf)
        crossing_peak = running_heads + state_max[:, None]
        row_max = jnp.maximum(crossing_peak, lax.optimization_barrier(jnp.max(pair_log, axis=2)))
        scores = jnp.einsum('thd,shd->hts', query_wide, block_key.astype(jnp.float32)) * key_scale
        cell_weight = jnp.exp(pair_log - row_max[:, :, None]) * scores
        weight_low = lax.optimization_barrier(cell_weight.astype(jnp.bfloat16)).astype(jnp.float32)
        inter_scale = jnp.exp(crossing_peak - row_max)
        read_state = jnp.einsum('thd,hde->hte', query_wide, state_matrix, precision=lax.Precision.HIGHEST)
        read_norm = jnp.einsum('thd,hd->ht', query_wide, state_norm, precision=lax.Precision.HIGHEST)
        numerator = inter_scale[:, :, None] * read_state + jnp.einsum('hts,she->hte', weight_low, value_wide)
        denominator = inter_scale * read_norm + lax.optimization_barrier(jnp.sum(cell_weight, axis=2))
        result = numerator / jnp.maximum(jnp.abs(denominator), jnp.exp(-row_max))[:, :, None]
        new_max = jnp.maximum(block_decay + state_max, block_max)
        keep_scale = jnp.exp(block_decay + state_max - new_max)
        add_scale = jnp.exp(block_max - new_max)
        new_matrix = keep_scale[:, None, None] * state_matrix + add_scale[:, None, None] * block_matrix
        new_norm = keep_scale[:, None] * state_norm + add_scale[:, None] * block_norm
        return ((new_matrix, new_norm, new_max), jnp.transpose(result, (1, 0, 2)))
    start_state = (jnp.zeros((head_count, key_dim, value_dim), jnp.float32), jnp.zeros((head_count, key_dim), jnp.float32), jnp.full((head_count,), max_floor, jnp.float32))
    _, results = lax.scan(block_step, start_state, pieces_all)
    return results.reshape(seq_len, head_count, value_dim)

def routed_experts(normed, w_gate, w_up, w_down, routes, route_weight):
    token_count, model_width = normed.shape
    expert_count = w_gate.shape[0]
    top_count = routes.shape[1]
    assign_count = token_count * top_count
    flat_expert = routes.reshape(assign_count).astype(jnp.int32)
    order = jnp.argsort(flat_expert, stable=True).astype(jnp.int32)
    sorted_expert = flat_expert[order]
    counts = jnp.zeros((expert_count,), jnp.int32).at[flat_expert].add(1)
    padded = ((counts + block_rows - 1) // block_rows * block_rows).astype(jnp.int32)
    pad_end = jnp.cumsum(padded).astype(jnp.int32)
    pad_start = (pad_end - padded).astype(jnp.int32)
    first_of = (jnp.cumsum(counts).astype(jnp.int32) - counts).astype(jnp.int32)
    destination = (pad_start[sorted_expert] + jnp.arange(assign_count, dtype=jnp.int32) - first_of[sorted_expert]).astype(jnp.int32)
    slot_total = (assign_count + expert_count * (block_rows - 1) + block_rows - 1) // block_rows * block_rows
    block_total = slot_total // block_rows
    flat_token = jnp.arange(assign_count, dtype=jnp.int32) // top_count
    slot_token = jnp.zeros((slot_total,), jnp.int32).at[destination].set(flat_token[order])
    block_expert = jnp.minimum(jnp.searchsorted(pad_end, jnp.arange(block_total, dtype=jnp.int32) * block_rows, side='right'), expert_count - 1).astype(jnp.int32)
    block_inputs = normed[slot_token].reshape(block_total, block_rows, model_width)

    def one_block(operands):
        block_input, expert_id = operands
        gate_part = jnp.dot(block_input, w_gate[expert_id], preferred_element_type=jnp.float32)
        up_part = jnp.dot(block_input, w_up[expert_id], preferred_element_type=jnp.float32)
        hidden = (jax.nn.silu(gate_part) * up_part).astype(jnp.bfloat16)
        return jnp.dot(hidden, w_down[expert_id], preferred_element_type=jnp.float32).astype(jnp.bfloat16)
    block_outputs = lax.map(one_block, (block_inputs, block_expert)).reshape(slot_total, model_width)
    sorted_outputs = block_outputs[destination]
    assigned = jnp.zeros((assign_count, model_width), jnp.bfloat16).at[order].set(sorted_outputs)
    weighted = assigned.astype(jnp.float32).reshape(token_count, top_count, model_width) * route_weight[:, :, None]
    return lax.optimization_barrier(jnp.sum(weighted, axis=1))

def reference(residual, queries, keys, values, out_gate, in_gate, forget_gate, head_gain, w_out, norm_gain, shared_gate, shared_up, shared_down, w_gate, w_up, w_down, routes, route_weight):
    query_heads = queries.reshape(TOKENS, MEMORY_SPLITS, DQK)
    key_heads = keys.reshape(TOKENS, MEMORY_SPLITS, DQK)
    value_heads = values.reshape(TOKENS, MEMORY_SPLITS, DV)
    log_forget = jax.nn.log_sigmoid(forget_gate)
    forward_out = direction_pass(query_heads, key_heads, value_heads, in_gate[0], log_forget[0], TOK_DEV)
    backward_out = direction_pass(query_heads[::-1], key_heads[::-1], value_heads[::-1], in_gate[1][::-1], log_forget[1][::-1], TOK_DEV)[::-1]
    summed = forward_out + backward_out
    normal = summed * lax.rsqrt(lax.optimization_barrier(jnp.mean(summed * summed, axis=-1, keepdims=True)) + epsilon)
    mixed_heads = (normal.reshape(TOKENS, MEMORY_SPLITS * DV) * head_gain * jax.nn.sigmoid(out_gate.astype(jnp.float32))).astype(jnp.bfloat16)
    projected = jnp.dot(mixed_heads, w_out, preferred_element_type=jnp.float32)
    updated = (residual.astype(jnp.float32) + projected).astype(jnp.bfloat16)
    updated_wide = updated.astype(jnp.float32)
    normed = (updated_wide * lax.rsqrt(lax.optimization_barrier(jnp.mean(updated_wide * updated_wide, axis=-1, keepdims=True)) + epsilon) * norm_gain).astype(jnp.bfloat16)
    shared_expert_hidden = (jax.nn.silu(jnp.dot(normed, shared_gate, preferred_element_type=jnp.float32)) * jnp.dot(normed, shared_up, preferred_element_type=jnp.float32)).astype(jnp.bfloat16)
    shared = jnp.dot(shared_expert_hidden, shared_down, preferred_element_type=jnp.float32)
    routed = routed_experts(normed, w_gate, w_up, w_down, routes, route_weight)
    return (updated_wide + shared + routed).astype(jnp.bfloat16)
```

```python
import functools
import math

import jax
import jax.numpy as jnp
from jax import lax
from jax.experimental import pallas as pl
from jax.experimental.pallas import tpu as pltpu
from jax.sharding import Mesh
from jax.sharding import PartitionSpec as P

SP = ("sp_0", "sp_1", "sp_2")
SP_TP = ("sp_0", "sp_1", "sp_2", "tp")
MESH = pl.DeviceIdType.MESH

epsilon = 1e-06
max_floor = -1e30
f32 = jnp.float32
bf16 = jnp.bfloat16

NT = (((1,), (1,)), ((), ()))
TN = (((0,), (0,)), ((), ()))
NN = (((1,), (0,)), ((), ()))


def exact(a, b, dims):
    return lax.dot_general(
        a, b, dims, precision=lax.Precision.HIGHEST, preferred_element_type=f32
    )


def mul(a, b, dims=NN):
    return lax.dot_general(a, b, dims, preferred_element_type=f32)


def here():
    return tuple(lax.axis_index(a) for a in SP_TP)


def spots():
    return tuple(lax.axis_size(a) for a in SP_TP)


def flat(at, sizes):
    number = at[0]
    for part, size in zip(at[1:], sizes[1:]):
        number = number * size + part
    return number


def away(step, sign):
    at, sizes = here(), spots()
    out = []
    rest = step
    for part, size in reversed(list(zip(at, sizes))):
        move = lax.rem(rest, size)
        rest = rest // size
        out.append(lax.rem(part + (move if sign > 0 else size - move), size))
    return tuple(reversed(out))


def mixer_kernel(
    heads,
    key_dim,
    value_dim,
    gates_ref,
    gain_ref,
    norm_gain_ref,
    q_hbm,
    k_hbm,
    v_hbm,
    og_hbm,
    res_hbm,
    wout_hbm,
    updated_ref,
    normed_ref,
    q,
    k,
    v,
    og,
    res,
    wout,
    out_m,
    in_m,
    back_m,
    state_m,
    out_a,
    in_a,
    back_a,
    state_a,
    local,
    mixed,
    proj_out,
    proj_in,
    proj_own,
    load_sem,
    send_sem,
    recv_sem,
    pair_sem,
):
    sizes = spots()
    places = sizes[0] * sizes[1] * sizes[2]
    z, y, x, core = here()
    me = flat((z, y, x), sizes[:3])
    rows = q.shape[0]
    units = 2 * heads
    chunks = places // units
    piece = out_m.shape[1]
    key_scale = 1.0 / math.sqrt(key_dim)

    loads = [
        pltpu.make_async_copy(a, b, load_sem.at[n])
        for n, (a, b) in enumerate(
            [(k_hbm, k), (v_hbm, v), (q_hbm, q), (og_hbm, og), (res_hbm, res), (wout_hbm, wout)]
        )
    ]
    for load in loads:
        load.start()

    barrier = pltpu.get_barrier_semaphore()
    two = sizes[3]

    def greet(step, carry):
        pl.semaphore_signal(barrier, inc=1, device_id=away(step * two, 1), device_id_type=MESH)
        return carry

    lax.fori_loop(1, places, greet, 0)
    partner = (z, y, x, lax.rem(core + 1, two))
    pl.semaphore_signal(barrier, inc=1, device_id=partner, device_id_type=MESH)

    ig = gates_ref[0:units, :]
    decay = jnp.exp(-gates_ref[units : 2 * units, :])
    up = 1.0 + decay
    lf = -jnp.where(up == 1.0, decay, jnp.log(up) * (decay / jnp.where(up == 1.0, 1.0, up - 1.0)))

    line = lax.broadcasted_iota(jnp.int32, (rows, rows), 0)
    lane = lax.broadcasted_iota(jnp.int32, (rows, rows), 1)
    upper = (line <= lane).astype(f32)
    lower = (line >= lane).astype(f32)
    eye = (line == lane).astype(f32)
    first_row = lax.broadcasted_iota(jnp.int32, (units, rows), 0) < heads
    first_col = lax.broadcasted_iota(jnp.int32, (rows, units), 1) < heads
    run_row = jnp.where(first_row, exact(lf, upper, NN), exact(lf, lower, NN))
    run_col = jnp.where(first_col, exact(lower, lf, NT), exact(upper, lf, NT))
    ig_col = exact(eye, ig, NT)
    total_col = jnp.where(first_col[0:1], run_col[rows - 1 : rows, :], run_col[0:1, :])
    a_col = total_col - run_col + ig_col
    peak_col = jnp.max(a_col, axis=0, keepdims=True)
    scale_col = jnp.exp(a_col - peak_col) * key_scale

    loads[0].wait()
    loads[1].wait()
    for unit in range(units):
        h = unit % heads
        kh = k[:, h * key_dim : (h + 1) * key_dim].astype(f32)
        low = (kh * scale_col[:, unit : unit + 1]).astype(bf16)
        matrix = mul(low, v[:, h * value_dim : (h + 1) * value_dim], TN)
        out_m[unit * chunks : (unit + 1) * chunks] = matrix.astype(bf16).reshape(
            chunks, piece, value_dim
        )
        norm = jnp.sum(low.astype(f32), axis=0, keepdims=True)
        out_a[unit, 0:1, :] = norm
        out_a[unit, 1:2, :] = jnp.broadcast_to(peak_col[:, unit : unit + 1], (1, key_dim))
        out_a[unit, 2:3, :] = jnp.broadcast_to(total_col[:, unit : unit + 1], (1, key_dim))

    pl.semaphore_wait(barrier, places)

    def exchange(round_at, src_m, dst_m, src_a, dst_a, a_of):
        def copies(step, sign):
            other = away(step * two, sign)
            spot = flat(other[:3], sizes[:3])
            return [
                pltpu.make_async_remote_copy(
                    src_ref=src_m.at[spot],
                    dst_ref=dst_m.at[me],
                    send_sem=send_sem.at[round_at, 0, step],
                    recv_sem=recv_sem.at[round_at, 0, step],
                    device_id=other,
                    device_id_type=MESH,
                ),
                pltpu.make_async_remote_copy(
                    src_ref=src_a.at[a_of(spot)],
                    dst_ref=dst_a.at[me],
                    send_sem=send_sem.at[round_at, 1, step],
                    recv_sem=recv_sem.at[round_at, 1, step],
                    device_id=other,
                    device_id_type=MESH,
                ),
            ]

        def go(i, carry):
            for copy in copies(lax.rem(i * 27, places), 1):
                copy.start()
            return carry

        lax.fori_loop(1, places, go, 0)
        dst_m[me] = src_m[me]
        dst_a[me] = src_a[a_of(me)]

        def finish(i, carry):
            step = lax.rem(i * 27, places)
            source = away(step * two, -1)
            spot = flat(source[:3], sizes[:3])
            pltpu.make_async_copy(
                src_m.at[spot], dst_m.at[spot], recv_sem.at[round_at, 0, step]
            ).wait()
            pltpu.make_async_copy(
                src_a.at[a_of(spot)], dst_a.at[spot], recv_sem.at[round_at, 1, step]
            ).wait()
            for copy in copies(step, 1):
                copy.wait_send()
            return carry

        return lambda: lax.fori_loop(1, places, finish, 0)

    arrive = exchange(0, out_m, in_m, out_a, in_a, lambda spot: spot // chunks)

    loads[2].wait()
    peaks, sums = [], []
    for h in range(heads):
        qh = q[:, h * key_dim : (h + 1) * key_dim]
        kh = k[:, h * key_dim : (h + 1) * key_dim]
        vh = v[:, h * value_dim : (h + 1) * value_dim]
        scores = mul(qh, kh, NT) * key_scale
        for way in range(2):
            unit = way * heads + h
            seen = (line >= lane) if way == 0 else (line <= lane)
            pair = run_col[:, unit : unit + 1] + (ig[unit : unit + 1] - run_row[unit : unit + 1])
            pair = jnp.where(seen, pair, max_floor)
            top = jnp.max(pair, axis=1, keepdims=True)
            weight = jnp.where(seen, jnp.exp(pair - top), 0.0) * scores
            local[unit] = mul(weight.astype(bf16), vh)
            peaks.append(top)
            sums.append(jnp.sum(weight, axis=1, keepdims=True))

    arrive()
    backward = me // (chunks * heads)

    def advance(s, carry):
        m, n, top = carry
        at = s + backward * (places - 1 - 2 * s)
        back_m[at] = m.astype(bf16)
        back_a[at, 0:1, :] = n
        back_a[at, 1:2, :] = top
        block_top = in_a[at, 1:2, :]
        moved = in_a[at, 2:3, :] + top
        new = jnp.maximum(moved, block_top)
        keep = jnp.exp(moved - new)
        add = jnp.exp(block_top - new)
        wide_keep = jnp.concatenate([keep] * (value_dim // key_dim), axis=1)
        wide_add = jnp.concatenate([add] * (value_dim // key_dim), axis=1)
        m = wide_keep * m + wide_add * in_m[at].astype(f32)
        n = keep * n + add * in_a[at, 0:1, :]
        return m, n, new

    lax.fori_loop(
        0,
        places,
        advance,
        (
            jnp.zeros((piece, value_dim), f32),
            jnp.zeros((1, key_dim), f32),
            jnp.full((1, key_dim), max_floor, f32),
        ),
    )
    arrive = exchange(1, back_m, state_m, back_a, state_a, lambda spot: spot)
    loads[3].wait()
    arrive()

    for h in range(heads):
        qh = q[:, h * key_dim : (h + 1) * key_dim]
        qw = qh.astype(f32)
        total = None
        for way in range(2):
            unit = way * heads + h
            state = state_m[unit * chunks : (unit + 1) * chunks].reshape(key_dim, value_dim)
            norm = state_a[unit * chunks, 0:1, :]
            top = state_a[unit * chunks, 1:2, :]
            crossing = run_col[:, unit : unit + 1] + top[:, 0:1]
            row_max = jnp.maximum(crossing, peaks[h * 2 + way])
            carry = jnp.exp(crossing - row_max)
            inner = jnp.exp(peaks[h * 2 + way] - row_max)
            read_norm = jnp.sum(qw * norm, axis=1, keepdims=True)
            divisor = carry * read_norm + inner * sums[h * 2 + way]
            divisor = jnp.maximum(jnp.abs(divisor), jnp.exp(-row_max))
            part = (carry * mul(qh, state) + inner * local[unit]) / divisor
            total = part if total is None else total + part
        normal = total * lax.rsqrt(jnp.mean(total * total, axis=1, keepdims=True) + epsilon)
        span = slice(h * value_dim, (h + 1) * value_dim)
        gate = 1.0 / (1.0 + jnp.exp(-og[:, span].astype(f32)))
        mixed[:, span] = (normal * gain_ref[:, span] * gate).astype(bf16)

    loads[4].wait()
    loads[5].wait()
    half = res.shape[0]
    width = res.shape[1]
    tile = 512
    theirs = pl.ds(pl.multiple_of((1 - core) * half, half), half)
    mine = pl.ds(pl.multiple_of(core * half, half), half)

    def project(n, carry, span, ref):
        cols = pl.ds(pl.multiple_of(n * tile, tile), tile)
        ref[:, cols] = mul(mixed[span, :], wout[:, cols]).astype(ref.dtype)
        return carry

    lax.fori_loop(0, width // tile, functools.partial(project, span=theirs, ref=proj_out), 0)
    trade = pltpu.make_async_remote_copy(
        src_ref=proj_out,
        dst_ref=proj_in,
        send_sem=pair_sem.at[0],
        recv_sem=pair_sem.at[1],
        device_id=partner,
        device_id_type=MESH,
    )
    trade.start()
    lax.fori_loop(0, width // tile, functools.partial(project, span=mine, ref=proj_own), 0)
    trade.wait()
    updated = (res[...].astype(f32) + (proj_own[...] + proj_in[...].astype(f32))).astype(bf16)
    updated_ref[...] = updated
    wide = updated.astype(f32)
    normed_ref[...] = (
        wide
        * lax.rsqrt(jnp.mean(wide * wide, axis=1, keepdims=True) + epsilon)
        * norm_gain_ref[...]
    ).astype(bf16)


def mixer(residual, queries, keys, values, out_gate, gates, head_gain, w_out, norm_gain):
    rows, query_width = queries.shape
    heads = gates.shape[0] // 4
    key_dim, value_dim = query_width // heads, values.shape[1] // heads
    places = math.prod(lax.axis_size(a) for a in SP)
    units = 2 * heads
    piece = key_dim * units // places
    half, width = residual.shape
    vmem = pl.BlockSpec(memory_space=pltpu.VMEM)
    hbm = pl.BlockSpec(memory_space=pl.ANY)
    matrices = pltpu.VMEM((places, piece, value_dim), bf16)
    extras = pltpu.VMEM((places, 4, key_dim), f32)
    return pl.pallas_call(
        functools.partial(mixer_kernel, heads, key_dim, value_dim),
        out_shape=[jax.ShapeDtypeStruct((half, width), bf16)] * 2,
        in_specs=[vmem] * 3 + [hbm] * 6,
        out_specs=[vmem] * 2,
        scratch_shapes=[
            pltpu.VMEM(queries.shape, bf16),
            pltpu.VMEM(keys.shape, bf16),
            pltpu.VMEM(values.shape, bf16),
            pltpu.VMEM(out_gate.shape, bf16),
            pltpu.VMEM(residual.shape, bf16),
            pltpu.VMEM(w_out.shape, bf16),
            matrices,
            matrices,
            matrices,
            matrices,
            pltpu.VMEM((units, 4, key_dim), f32),
            extras,
            extras,
            extras,
            pltpu.VMEM((units, rows, value_dim), f32),
            pltpu.VMEM(values.shape, bf16),
            pltpu.VMEM((half, width), bf16),
            pltpu.VMEM((half, width), bf16),
            pltpu.VMEM((half, width), f32),
            pltpu.SemaphoreType.DMA((6,)),
            pltpu.SemaphoreType.DMA((2, 2, places)),
            pltpu.SemaphoreType.DMA((2, 2, places)),
            pltpu.SemaphoreType.DMA((2,)),
        ],
        compiler_params=pltpu.CompilerParams(
            collective_id=0, has_side_effects=True, vmem_limit_bytes=48 * 1024 * 1024
        ),
        name="mixer",
    )(
        gates,
        head_gain.reshape(1, -1),
        norm_gain.reshape(1, -1),
        queries,
        keys,
        values,
        out_gate,
        residual,
        w_out,
    )


def silu(value):
    return value / (1.0 + jnp.exp(-value))


def experts_kernel(
    slots,
    group,
    stride,
    normed,
    updated,
    routes_row,
    routes_col,
    weight_col,
    sg_hbm,
    su_hbm,
    sd_hbm,
    wg_hbm,
    wu_hbm,
    wd_hbm,
    out_ref,
    sg,
    su,
    sd,
    wg,
    wu,
    wd,
    outgoing,
    arrived,
    returned,
    packed,
    answer,
    hidden,
    shared_hidden,
    total,
    load_sem,
    send_sem,
    recv_sem,
    send_back,
    recv_back,
):
    sizes = spots()
    count = math.prod(sizes)
    me = flat(here(), sizes)
    tokens, width = normed.shape
    top = routes_row.shape[0]
    tile = 512

    loads = [
        pltpu.make_async_copy(a, b, load_sem.at[n])
        for n, (a, b) in enumerate(
            [
                (sg_hbm, sg),
                (su_hbm, su),
                (sd_hbm, sd),
                (wg_hbm.at[0], wg),
                (wu_hbm.at[0], wu),
                (wd_hbm.at[0], wd),
            ]
        )
    ]
    for load in loads:
        load.start()

    barrier = pltpu.get_barrier_semaphore()

    def greet(step, carry):
        pl.semaphore_signal(barrier, inc=1, device_id=away(step, 1), device_id_type=MESH)
        return carry

    lax.fori_loop(1, count, greet, 0)

    expert = lax.broadcasted_iota(jnp.int32, (count, tokens), 0)
    named = jnp.zeros((count, tokens), f32)
    for n in range(top):
        named = named + (expert == routes_row[n : n + 1, :]).astype(f32)
    earlier = (
        lax.broadcasted_iota(jnp.int32, (tokens, tokens), 0)
        < lax.broadcasted_iota(jnp.int32, (tokens, tokens), 1)
    ).astype(bf16)
    rank = mul(named.astype(bf16), earlier)
    rank = jnp.where(named > 0.0, rank, -1.0)
    total[:, 0:tokens] = rank
    block = 16

    def fill(b, carry):
        lines = pl.ds(pl.multiple_of(b * block, block), block)
        at = total[lines, 0:tokens]
        slot = lax.broadcasted_iota(jnp.int32, (block, slots, tokens), 1).astype(f32)
        pick = (at[:, None, :] == slot).astype(f32).reshape(block * slots, tokens)
        moved = mul(pick.astype(bf16), normed[...])
        outgoing[lines] = moved.reshape(block, slots, width).astype(bf16)
        return carry

    lax.fori_loop(0, count // block, fill, 0)
    pl.semaphore_wait(barrier, count - 1)

    def dispatch(i):
        other = away(lax.rem(i * stride, count), 1)
        return pltpu.make_async_remote_copy(
            src_ref=outgoing.at[flat(other, sizes)],
            dst_ref=arrived.at[i],
            send_sem=send_sem.at[i],
            recv_sem=recv_sem.at[i],
            device_id=other,
            device_id_type=MESH,
        )

    def give_back(i):
        source = away(lax.rem(i * stride, count), -1)
        return pltpu.make_async_remote_copy(
            src_ref=answer.at[i],
            dst_ref=returned.at[me],
            send_sem=send_back.at[i],
            recv_sem=recv_back.at[i],
            device_id=source,
            device_id_type=MESH,
        )

    def send(i, carry):
        dispatch(i).start()
        return carry

    lax.fori_loop(1, count, send, 0)
    arrived[0] = outgoing[me]

    for load in loads[:3]:
        load.wait()
    shared_hidden[...] = (silu(mul(normed[...], sg[...])) * mul(normed[...], su[...])).astype(bf16)

    def shared_part(n, carry):
        cols = pl.ds(pl.multiple_of(n * tile, tile), tile)
        total[:, cols] = updated[:, cols].astype(f32) + mul(shared_hidden[...], sd[:, cols])
        return carry

    lax.fori_loop(0, width // tile, shared_part, 0)

    for load in loads[3:]:
        load.wait()

    def work(g, carry):
        def landed(i, inner):
            dispatch(i).wait_recv()
            return inner

        lax.fori_loop(jnp.maximum(g * group, 1), (g + 1) * group, landed, 0)
        sources = pl.ds(pl.multiple_of(g * group, group), group)
        packed[...] = arrived[sources].astype(f32).reshape(group * slots, width).astype(bf16)
        hidden[...] = (silu(mul(packed[...], wg[...])) * mul(packed[...], wu[...])).astype(bf16)

        def down(n, inner):
            cols = pl.ds(pl.multiple_of(n * tile, tile), tile)
            answer[sources, :, cols] = (
                mul(hidden[...], wd[:, cols]).reshape(group, slots, tile).astype(bf16)
            )
            return inner

        lax.fori_loop(0, width // tile, down, 0)

        def reply(i, inner):
            give_back(i).start()
            return inner

        lax.fori_loop(jnp.maximum(g * group, 1), (g + 1) * group, reply, 0)
        return carry

    lax.fori_loop(0, count // group, work, 0)
    returned[me] = answer[0]

    def close(i, carry):
        dispatch(i).wait_send()
        give_back(i).wait_send()
        give_back(i).wait_recv()
        return carry

    lax.fori_loop(1, count, close, 0)

    span = count * slots
    lane = lax.broadcasted_iota(jnp.int32, (tokens, span), 1)
    owner = lane // slots
    marks = jnp.zeros((tokens, span), f32)
    share = jnp.zeros((tokens, span), f32)
    for n in range(top):
        hit = owner == routes_col[:, n : n + 1]
        marks = marks + hit.astype(f32)
        share = share + jnp.where(hit, weight_col[:, n : n + 1], 0.0)
    before = (
        lax.broadcasted_iota(jnp.int32, (tokens, tokens), 1)
        < lax.broadcasted_iota(jnp.int32, (tokens, tokens), 0)
    ).astype(bf16)
    order = mul(before, marks.astype(bf16))
    share = jnp.where(order == (lane - owner * slots).astype(f32), share, 0.0)
    high = share.astype(bf16)
    low = (share - high.astype(f32)).astype(bf16)

    def gather(n, carry):
        cols = pl.ds(pl.multiple_of(n * tile, tile), tile)
        rows = returned[:, :, cols].astype(f32).reshape(span, tile).astype(bf16)
        out_ref[:, cols] = (total[:, cols] + (mul(high, rows) + mul(low, rows))).astype(bf16)
        return carry

    lax.fori_loop(0, width // tile, gather, 0)


def experts(normed, updated, routes, weight, shared_gate, shared_up, shared_down, gate, up, down):
    tokens, width = normed.shape
    top = routes.shape[1]
    count = math.prod(lax.axis_size(a) for a in SP_TP)
    slots = tokens * top * lax.axis_size("tp") // count
    group = 32
    hidden = gate.shape[2]
    vmem = pl.BlockSpec(memory_space=pltpu.VMEM)
    hbm = pl.BlockSpec(memory_space=pl.ANY)
    rows = pltpu.VMEM((count, slots, width), bf16)
    return pl.pallas_call(
        functools.partial(experts_kernel, slots, group, 37),
        out_shape=jax.ShapeDtypeStruct((tokens, width), bf16),
        in_specs=[vmem] * 5 + [hbm] * 6,
        out_specs=vmem,
        scratch_shapes=[
            pltpu.VMEM(shared_gate.shape, bf16),
            pltpu.VMEM(shared_up.shape, bf16),
            pltpu.VMEM(shared_down.shape, bf16),
            pltpu.VMEM(gate.shape[1:], bf16),
            pltpu.VMEM(up.shape[1:], bf16),
            pltpu.VMEM(down.shape[1:], bf16),
            rows,
            rows,
            rows,
            pltpu.VMEM((group * slots, width), bf16),
            rows,
            pltpu.VMEM((group * slots, hidden), bf16),
            pltpu.VMEM((tokens, shared_gate.shape[1]), bf16),
            pltpu.VMEM((tokens, width), f32),
            pltpu.SemaphoreType.DMA((6,)),
            pltpu.SemaphoreType.DMA((count,)),
            pltpu.SemaphoreType.DMA((count,)),
            pltpu.SemaphoreType.DMA((count,)),
            pltpu.SemaphoreType.DMA((count,)),
        ],
        compiler_params=pltpu.CompilerParams(
            collective_id=1, has_side_effects=True, vmem_limit_bytes=60 * 1024 * 1024
        ),
        name="experts",
    )(
        normed,
        updated,
        routes.T,
        routes,
        weight,
        shared_gate,
        shared_up,
        shared_down,
        gate,
        up,
        down,
    )


def local(
    residual,
    queries,
    keys,
    values,
    out_gate,
    in_gate,
    forget_gate,
    head_gain,
    w_out,
    norm_gain,
    shared_gate,
    shared_up,
    shared_down,
    w_gate,
    w_up,
    w_down,
    routes,
    route_weight,
):
    gates = jnp.stack([in_gate, forget_gate]).transpose(0, 1, 3, 2)
    gates = gates.reshape(-1, in_gate.shape[1])
    updated, normed = mixer(
        residual, queries, keys, values, out_gate, gates, head_gain, w_out, norm_gain
    )
    return experts(
        normed,
        updated,
        routes,
        route_weight,
        shared_gate,
        shared_up,
        shared_down,
        w_gate,
        w_up,
        w_down,
    )


def solution(mesh):
    finer = Mesh(mesh.devices.reshape(4, 4, 4, mesh.shape["tp"]), SP_TP)
    return jax.shard_map(
        local,
        mesh=finer,
        in_specs=(
            P(SP_TP, None),
            P(SP, "tp"),
            P(SP, "tp"),
            P(SP, "tp"),
            P(SP, "tp"),
            P(None, SP, "tp"),
            P(None, SP, "tp"),
            P("tp"),
            P("tp", None),
            P(),
            P(),
            P(),
            P(),
            P(SP_TP, None, None),
            P(SP_TP, None, None),
            P(SP_TP, None, None),
            P(SP_TP, None),
            P(SP_TP, None),
        ),
        out_specs=P(SP_TP, None),
        check_vma=False,
    )
```

```python
import functools
import math

import jax
import jax.numpy as jnp
from jax import lax
from jax.experimental import pallas as pl
from jax.experimental.pallas import tpu as pltpu
from jax.sharding import Mesh
from jax.sharding import PartitionSpec as P

SP = ("sp_0", "sp_1", "sp_2")
SP_TP = ("sp_0", "sp_1", "sp_2", "tp")
MESH = pl.DeviceIdType.MESH

epsilon = 1e-06
max_floor = -1e30
f32 = jnp.float32
bf16 = jnp.bfloat16

NT = (((1,), (1,)), ((), ()))
TN = (((0,), (0,)), ((), ()))
NN = (((1,), (0,)), ((), ()))


def exact(a, b, dims):
    return lax.dot_general(
        a, b, dims, precision=lax.Precision.HIGHEST, preferred_element_type=f32
    )


def mul(a, b, dims=NN):
    return lax.dot_general(a, b, dims, preferred_element_type=f32)


def here():
    return tuple(lax.axis_index(a) for a in SP_TP)


def spots():
    return tuple(lax.axis_size(a) for a in SP_TP)


def flat(at, sizes):
    number = at[0]
    for part, size in zip(at[1:], sizes[1:]):
        number = number * size + part
    return number


def ring(at, size):
    return [at if move == 0 else lax.rem(at + move, size) for move in range(size)]


def hops(moves, sizes):
    return sum(min(move, size - move) for move, size in zip(moves, sizes))


def silu(value):
    return value / (1.0 + jnp.exp(-value))


def layer_kernel(
    heads,
    key_dim,
    value_dim,
    slots,
    group,
    ig_hbm,
    fg_hbm,
    routes_hbm,
    weight_hbm,
    gain_hbm,
    norm_gain_hbm,
    q_hbm,
    k_hbm,
    v_hbm,
    og_hbm,
    res_hbm,
    wout_hbm,
    sg_hbm,
    su_hbm,
    sd_hbm,
    wg_hbm,
    wu_hbm,
    wd_hbm,
    out_ref,
    in_gate,
    forget_gate,
    routes,
    route_weight,
    gain,
    norm_gain,
    q,
    k,
    v,
    og,
    res,
    wout,
    sg,
    su,
    sd,
    wg,
    wu,
    wd,
    out_m,
    in_m,
    back_m,
    state_m,
    out_a,
    in_a,
    back_a,
    state_a,
    local,
    mixed,
    proj_out,
    proj_in,
    proj_own,
    normed,
    rank_ref,
    weight_ref,
    share_high,
    share_low,
    outgoing,
    arrived,
    returned,
    packed,
    answer,
    hidden,
    shared_hidden,
    total_ref,
    gate_sem,
    load_sem,
    state_send,
    state_recv,
    pair_sem,
    send_sem,
    recv_sem,
    send_back,
    recv_back,
):
    sizes = spots()
    places = sizes[0] * sizes[1] * sizes[2]
    two = sizes[3]
    count = places * two
    z, y, x, core = here()
    me = flat((z, y, x), sizes[:3])
    rows = q.shape[0]
    units = 2 * heads
    chunks = places // units
    piece = out_m.shape[1]
    key_scale = 1.0 / math.sqrt(key_dim)
    half, width = res.shape
    tile = 512

    loads = [
        pltpu.make_async_copy(a, b, load_sem.at[n])
        for n, (a, b) in enumerate(
            [
                (k_hbm, k),
                (v_hbm, v),
                (q_hbm, q),
                (og_hbm, og),
                (gain_hbm, gain),
                (norm_gain_hbm, norm_gain),
                (res_hbm, res),
                (wout_hbm, wout),
                (sg_hbm, sg),
                (su_hbm, su),
                (sd_hbm, sd),
                (wg_hbm.at[0], wg),
                (wu_hbm.at[0], wu),
                (wd_hbm.at[0], wd),
                (routes_hbm, routes),
                (weight_hbm, route_weight),
            ]
        )
    ]
    gate_loads = [
        pltpu.make_async_copy(a, b, gate_sem.at[n])
        for n, (a, b) in enumerate([(ig_hbm, in_gate), (fg_hbm, forget_gate)])
    ]
    for load in gate_loads:
        load.start()
    for load in loads[:3]:
        load.start()

    barrier = pltpu.get_barrier_semaphore()
    zs, ys, xs, cores = (ring(at, size) for at, size in zip((z, y, x, core), sizes))
    moves = [
        (dz, dy, dx)
        for dz in range(sizes[0])
        for dy in range(sizes[1])
        for dx in range(sizes[2])
        if (dz, dy, dx) != (0, 0, 0)
    ]
    moves.sort(key=lambda move: (-hops(move, sizes), (move[0] + 2 * move[1] + 3 * move[2]) % 4))
    for dz, dy, dx in moves:
        pl.semaphore_signal(
            barrier, inc=1, device_id=(zs[dz], ys[dy], xs[dx], core), device_id_type=MESH
        )
    partner = (z, y, x, cores[1])
    pl.semaphore_signal(barrier, inc=1, device_id=partner, device_id_type=MESH)

    for load in gate_loads:
        load.wait()
    ig = jnp.concatenate([in_gate[0], in_gate[1]], axis=0)
    fg = jnp.concatenate([forget_gate[0], forget_gate[1]], axis=0)
    decay = jnp.exp(-fg)
    up = 1.0 + decay
    lf = -jnp.where(up == 1.0, decay, jnp.log(up) * (decay / jnp.where(up == 1.0, 1.0, up - 1.0)))
    line = lax.broadcasted_iota(jnp.int32, (rows, rows), 0)
    lane = lax.broadcasted_iota(jnp.int32, (rows, rows), 1)

    def sums_of(value, matrix):
        high = value.astype(bf16).astype(f32)
        middle = (value - high).astype(bf16).astype(f32)
        parts = jnp.concatenate([high, middle, value - high - middle], axis=0).astype(bf16)
        got = mul(parts, matrix.astype(f32).astype(bf16))
        return got[0:units] + (got[units : 2 * units] + got[2 * units :])

    first_row = lax.broadcasted_iota(jnp.int32, (units, rows), 0) < heads
    run_row = jnp.where(first_row, sums_of(lf, line <= lane), sums_of(lf, line >= lane))
    totals = jnp.where(first_row[:, 0:1], run_row[:, rows - 1 : rows], run_row[:, 0:1])
    a_row = totals - run_row + ig
    block_peak = jnp.max(a_row, axis=1, keepdims=True)
    scale_row = jnp.exp(a_row - block_peak) * key_scale
    turned = jnp.concatenate([run_row, scale_row], axis=0).T
    run_col, scale_col = turned[:, 0:units], turned[:, units:]

    loads[0].wait()
    loads[1].wait()
    for load in loads[3:8]:
        load.start()
    for unit in range(units):
        h = unit % heads
        kh = k[:, h * key_dim : (h + 1) * key_dim].astype(f32)
        low = (kh * scale_col[:, unit : unit + 1]).astype(bf16)
        matrix = mul(low, v[:, h * value_dim : (h + 1) * value_dim], TN)
        out_m[unit * chunks : (unit + 1) * chunks] = matrix.astype(bf16).reshape(
            chunks, piece, value_dim
        )
        norm = jnp.sum(low.astype(f32), axis=0, keepdims=True)
        out_a[unit, 0:1, :] = norm
        out_a[unit, 1:2, :] = jnp.broadcast_to(block_peak[unit : unit + 1], (1, key_dim))
        out_a[unit, 2:3, :] = jnp.broadcast_to(totals[unit : unit + 1], (1, key_dim))
        out_a[unit, 3:4, :] = jnp.zeros((1, key_dim), f32)

    pl.semaphore_wait(barrier, places)

    def exchange(phase, src_m, dst_m, src_a, dst_a, a_src, a_dst, with_extra):
        extras = 0
        for dz, dy, dx in moves:
            other = (zs[dz], ys[dy], xs[dx], core)
            spot = flat(other[:3], sizes[:3])
            pairs = [(src_m.at[spot], dst_m.at[me])]
            if with_extra(dz, dy, dx):
                pairs.append((src_a.at[a_src(spot)], dst_a.at[a_dst(me)]))
                extras += 1
            for n, (src, dst) in enumerate(pairs):
                pltpu.make_async_remote_copy(
                    src_ref=src,
                    dst_ref=dst,
                    send_sem=state_send.at[phase, n],
                    recv_sem=state_recv.at[phase, n],
                    device_id=other,
                    device_id_type=MESH,
                ).start()
        dst_m[me] = src_m[me]
        dst_a[a_dst(me)] = src_a[a_src(me)]

        def all_of(sems):
            for n, (dst, number) in enumerate([(dst_m, places - 1), (dst_a, extras)]):
                part = dst.at[pl.ds(0, number)]
                pltpu.make_async_copy(part, part, sems.at[phase, n]).wait()

        return all_of

    first = exchange(
        0,
        out_m,
        in_m,
        out_a,
        in_a,
        lambda spot: spot // chunks,
        lambda spot: spot,
        lambda dz, dy, dx: True,
    )

    for load in loads[8:]:
        load.start()

    loads[2].wait()
    peaks, sums = [], []
    for h in range(heads):
        qh = q[:, h * key_dim : (h + 1) * key_dim]
        kh = k[:, h * key_dim : (h + 1) * key_dim]
        vh = v[:, h * value_dim : (h + 1) * value_dim]
        scores = mul(qh, kh, NT) * key_scale
        for way in range(2):
            unit = way * heads + h
            seen = (line >= lane) if way == 0 else (line <= lane)
            pair = run_col[:, unit : unit + 1] + (ig[unit : unit + 1] - run_row[unit : unit + 1])
            pair = jnp.where(seen, pair, max_floor)
            top = jnp.max(pair, axis=1, keepdims=True)
            weight = jnp.where(seen, jnp.exp(pair - top), 0.0) * scores
            local[unit] = mul(weight.astype(bf16), vh)
            peaks.append(top)
            sums.append(jnp.sum(weight, axis=1, keepdims=True))

    first(state_recv)
    backward = me // (chunks * heads)

    def advance(s, carry):
        m, n, top = carry
        at = s + backward * (places - 1 - 2 * s)
        back_m[at] = m.astype(bf16)
        back_a[at, 0:1, :] = n
        back_a[at, 1:2, :] = top
        block_top = in_a[at, 1:2, :]
        moved = in_a[at, 2:3, :] + top
        new = jnp.maximum(moved, block_top)
        keep = jnp.exp(moved - new)
        add = jnp.exp(block_top - new)
        wide_keep = jnp.concatenate([keep] * (value_dim // key_dim), axis=1)
        wide_add = jnp.concatenate([add] * (value_dim // key_dim), axis=1)
        m = wide_keep * m + wide_add * in_m[at].astype(f32)
        n = keep * n + add * in_a[at, 0:1, :]
        return m, n, new

    lax.fori_loop(
        0,
        places,
        advance,
        (
            jnp.zeros((piece, value_dim), f32),
            jnp.zeros((1, key_dim), f32),
            jnp.full((1, key_dim), max_floor, f32),
        ),
        unroll=4,
    )
    second = exchange(
        1,
        back_m,
        state_m,
        back_a,
        state_a,
        lambda spot: spot,
        lambda spot: spot // chunks,
        lambda dz, dy, dx: (dy * sizes[2] + dx) % chunks == 0,
    )

    for load in loads[14:]:
        load.wait()

    expert = lax.broadcasted_iota(jnp.int32, (count, half), 0)
    named = jnp.zeros((count, half), f32)
    share = jnp.zeros((count, half), f32)
    for n in range(routes.shape[0]):
        hit = expert == routes[n : n + 1, :]
        named = named + hit.astype(f32)
        share = share + jnp.where(hit, route_weight[n : n + 1, :], 0.0)
    earlier = (
        lax.broadcasted_iota(jnp.int32, (half, half), 0)
        < lax.broadcasted_iota(jnp.int32, (half, half), 1)
    ).astype(bf16)
    rank_ref[...] = jnp.where(named > 0.0, mul(named.astype(bf16), earlier), -1.0)
    weight_ref[...] = share
    block = group
    slot = lax.broadcasted_iota(jnp.int32, (block, slots, half), 1).astype(f32)

    def peers(b, sign):
        outer, inner = b // two, lax.rem(b, two) * two

        if sign < 0:
            zb = [lax.rem(z + 2 * sizes[0] - (outer + m), sizes[0]) for m in range(sizes[0])]
            yb = [lax.rem(y + 2 * sizes[1] - (inner + m), sizes[1]) for m in range(sizes[1])]
        else:
            zb = [lax.rem(z + outer + m, sizes[0]) for m in range(sizes[0])]
            yb = [lax.rem(y + inner + m, sizes[1]) for m in range(sizes[1])]
        out = []
        for n in range(block):
            dc, dx, rest = n % two, (n // two) % sizes[2], n // (two * sizes[2])
            dz = (2 * dx + dc) % sizes[0]
            dy = (rest + dx + 2 * dc) % sizes[1]
            out.append((zb[dz], yb[dy], xs[dx if sign > 0 else -dx], cores[dc]))
        return out

    def lines_of(ref, b):
        at = [flat(peer, sizes) for peer in peers(b, 1)]
        return jnp.concatenate([ref[pl.ds(one, 1), :] for one in at], axis=0)

    def picks(b):
        return (lines_of(rank_ref, b)[:, None, :] == slot).astype(f32)

    def sharing(b, carry):
        weights = picks(b) * lines_of(weight_ref, b)[:, None, :]
        turned = weights.reshape(block * slots, half).T
        high = turned.astype(bf16)
        share_high[b] = high
        share_low[b] = (turned - high.astype(f32)).astype(bf16)
        return carry

    lax.fori_loop(0, count // block, sharing, 0)

    loads[3].wait()
    loads[4].wait()
    second(state_recv)

    for h in range(heads):
        qh = q[:, h * key_dim : (h + 1) * key_dim]
        qw = qh.astype(f32)
        total = None
        for way in range(2):
            unit = way * heads + h
            state = state_m[unit * chunks : (unit + 1) * chunks].reshape(key_dim, value_dim)
            norm = state_a[unit, 0:1, :]
            top = state_a[unit, 1:2, :]
            crossing = run_col[:, unit : unit + 1] + top[:, 0:1]
            row_max = jnp.maximum(crossing, peaks[h * 2 + way])
            carry = jnp.exp(crossing - row_max)
            inner = jnp.exp(peaks[h * 2 + way] - row_max)
            read_norm = jnp.sum(qw * norm, axis=1, keepdims=True)
            divisor = carry * read_norm + inner * sums[h * 2 + way]
            divisor = jnp.maximum(jnp.abs(divisor), jnp.exp(-row_max))
            part = (carry * mul(qh, state) + inner * local[unit]) / divisor
            total = part if total is None else total + part
        normal = total * lax.rsqrt(jnp.mean(total * total, axis=1, keepdims=True) + epsilon)
        span = slice(h * value_dim, (h + 1) * value_dim)
        gate = 1.0 / (1.0 + jnp.exp(-og[:, span].astype(f32)))
        mixed[:, span] = (normal * gain[:, span] * gate).astype(bf16)

    for load in loads[5:8]:
        load.wait()
    tiles = [slice(n * tile, (n + 1) * tile) for n in range(width // tile)]
    trades = []
    for n, cols in enumerate(tiles):
        both = mul(mixed[...], wout[:, cols])
        proj_out[n] = jnp.where(core == 0, both[half:], both[:half]).astype(bf16)
        trades.append(
            pltpu.make_async_remote_copy(
                src_ref=proj_out.at[n],
                dst_ref=proj_in.at[n],
                send_sem=pair_sem.at[0, n],
                recv_sem=pair_sem.at[1, n],
                device_id=partner,
                device_id_type=MESH,
            )
        )
        trades[-1].start()
        own = jnp.where(core == 0, both[:half], both[half:])
        proj_own[:, cols] = res[:, cols].astype(f32) + own
    squares = jnp.zeros((half, 1), f32)
    for n, cols in enumerate(tiles):
        trades[n].wait()
        wide = (proj_own[:, cols] + proj_in[n].astype(f32)).astype(bf16).astype(f32)
        total_ref[:, cols] = wide
        squares = squares + jnp.sum(wide * wide, axis=1, keepdims=True)
    level = lax.rsqrt(squares * (1.0 / width) + epsilon)
    for cols in tiles:
        normed[:, cols] = (total_ref[:, cols] * level * norm_gain[:, cols]).astype(bf16)

    def dispatch(b, n, other):
        i = b * block + n
        return pltpu.make_async_remote_copy(
            src_ref=outgoing.at[i],
            dst_ref=arrived.at[i],
            send_sem=send_sem,
            recv_sem=recv_sem.at[b],
            device_id=other,
            device_id_type=MESH,
        )

    def give_back(b, n, other):
        i = b * block + n
        return pltpu.make_async_remote_copy(
            src_ref=answer.at[i],
            dst_ref=returned.at[i],
            send_sem=send_back,
            recv_sem=recv_back.at[b],
            device_id=other,
            device_id_type=MESH,
        )

    def start_all(b, copy, sign):
        others = peers(b, sign)

        @pl.when(b > 0)
        def _():
            copy(b, 0, others[0]).start()

        for n in range(1, block):
            copy(b, n, others[n]).start()

    def bytes_of(rows_ref, sem):
        pltpu.make_async_copy(rows_ref, rows_ref, sem).wait()

    def landed(b, sems, rows_ref):
        @pl.when(b == 0)
        def _():
            bytes_of(rows_ref.at[pl.ds(1, block - 1)], sems.at[0])

        @pl.when(b > 0)
        def _():
            bytes_of(rows_ref.at[pl.ds(b * block, block)], sems.at[b])

    def fill(b, carry):
        lines = pl.ds(pl.multiple_of(b * block, block), block)
        pick = picks(b).reshape(block * slots, half).astype(bf16)
        moved = mul(pick, normed[...])
        outgoing[lines] = moved.reshape(block, slots, width).astype(bf16)
        start_all(b, dispatch, 1)
        return carry

    lax.fori_loop(0, count // block, fill, 0)
    arrived[0] = outgoing[0]

    for load in loads[8:11]:
        load.wait()
    shared_hidden[...] = (silu(mul(normed[...], sg[...])) * mul(normed[...], su[...])).astype(bf16)

    def shared_part(n, carry):
        cols = pl.ds(pl.multiple_of(n * tile, tile), tile)
        total_ref[:, cols] = total_ref[:, cols] + mul(shared_hidden[...], sd[:, cols])
        return carry

    lax.fori_loop(0, width // tile, shared_part, 0)
    for load in loads[11:14]:
        load.wait()

    def work(g, carry):
        landed(g, recv_sem, arrived)
        sources = pl.ds(pl.multiple_of(g * group, group), group)
        packed[...] = arrived[sources].astype(f32).reshape(group * slots, width).astype(bf16)
        hidden[...] = (silu(mul(packed[...], wg[...])) * mul(packed[...], wu[...])).astype(bf16)

        def down(n, inner):
            cols = pl.ds(pl.multiple_of(n * tile, tile), tile)
            answer[sources, :, cols] = (
                mul(hidden[...], wd[:, cols]).reshape(group, slots, tile).astype(bf16)
            )
            return inner

        lax.fori_loop(0, width // tile, down, 0)
        start_all(g, give_back, -1)
        return carry

    lax.fori_loop(0, count // group, work, 0)
    returned[0] = answer[0]

    def collect(b, carry):
        landed(b, recv_back, returned)
        lines = pl.ds(pl.multiple_of(b * block, block), block)

        def part(n, inner):
            cols = pl.ds(pl.multiple_of(n * tile, tile), tile)
            landed = returned[lines, :, cols].astype(f32).reshape(block * slots, tile).astype(bf16)
            total_ref[:, cols] = total_ref[:, cols] + (
                mul(share_high[b], landed) + mul(share_low[b], landed)
            )
            return inner

        lax.fori_loop(0, width // tile, part, 0)
        return carry

    lax.fori_loop(0, count // block, collect, 0)
    out_ref[...] = total_ref[...].astype(bf16)

    bytes_of(outgoing.at[pl.ds(1, count - 1)], send_sem)
    bytes_of(answer.at[pl.ds(1, count - 1)], send_back)
    first(state_send)
    second(state_send)


def local(
    residual,
    queries,
    keys,
    values,
    out_gate,
    in_gate,
    forget_gate,
    head_gain,
    w_out,
    norm_gain,
    shared_gate,
    shared_up,
    shared_down,
    w_gate,
    w_up,
    w_down,
    routes,
    route_weight,
):
    rows = queries.shape[0]
    heads = in_gate.shape[2]
    key_dim, value_dim = queries.shape[1] // heads, values.shape[1] // heads
    places = math.prod(lax.axis_size(a) for a in SP)
    count = places * lax.axis_size("tp")
    units = 2 * heads
    piece = key_dim * units // places
    half, width = residual.shape
    slots = half * routes.shape[1] * lax.axis_size("tp") // count
    group = 16
    block = 16
    hidden = w_gate.shape[2]
    vmem = pl.BlockSpec(memory_space=pltpu.VMEM)
    hbm = pl.BlockSpec(memory_space=pltpu.HBM)
    matrices = pltpu.VMEM((places, piece, value_dim), bf16)
    extras = pltpu.VMEM((places, 4, key_dim), f32)
    slot_rows = pltpu.VMEM((count, slots, width), bf16)
    return pl.pallas_call(
        functools.partial(layer_kernel, heads, key_dim, value_dim, slots, group),
        out_shape=pltpu.VMEM((half, width), bf16),
        in_specs=[hbm] * 18,
        out_specs=vmem,
        scratch_shapes=[
            pltpu.VMEM((2, heads, rows), f32),
            pltpu.VMEM((2, heads, rows), f32),
            pltpu.VMEM((routes.shape[1], half), jnp.int32),
            pltpu.VMEM((routes.shape[1], half), f32),
            pltpu.VMEM((1, head_gain.shape[0]), f32),
            pltpu.VMEM((1, width), f32),
            pltpu.VMEM(queries.shape, bf16),
            pltpu.VMEM(keys.shape, bf16),
            pltpu.VMEM(values.shape, bf16),
            pltpu.VMEM(out_gate.shape, bf16),
            pltpu.VMEM(residual.shape, bf16),
            pltpu.VMEM(w_out.shape, bf16),
            pltpu.VMEM(shared_gate.shape, bf16),
            pltpu.VMEM(shared_up.shape, bf16),
            pltpu.VMEM(shared_down.shape, bf16),
            pltpu.VMEM(w_gate.shape[1:], bf16),
            pltpu.VMEM(w_up.shape[1:], bf16),
            pltpu.VMEM(w_down.shape[1:], bf16),
            matrices,
            matrices,
            matrices,
            matrices,
            pltpu.VMEM((units, 4, key_dim), f32),
            extras,
            extras,
            pltpu.VMEM((units, 4, key_dim), f32),
            pltpu.VMEM((units, rows, value_dim), f32),
            pltpu.VMEM(values.shape, bf16),
            pltpu.VMEM((width // 512, half, 512), bf16),
            pltpu.VMEM((width // 512, half, 512), bf16),
            pltpu.VMEM((half, width), f32),
            pltpu.VMEM((half, width), bf16),
            pltpu.VMEM((count, half), f32),
            pltpu.VMEM((count, half), f32),
            pltpu.VMEM((count // block, half, block * slots), bf16),
            pltpu.VMEM((count // block, half, block * slots), bf16),
            slot_rows,
            slot_rows,
            slot_rows,
            pltpu.VMEM((group * slots, width), bf16),
            slot_rows,
            pltpu.VMEM((group * slots, hidden), bf16),
            pltpu.VMEM((half, shared_gate.shape[1]), bf16),
            pltpu.VMEM((half, width), f32),
            pltpu.SemaphoreType.DMA((2,)),
            pltpu.SemaphoreType.DMA((16,)),
            pltpu.SemaphoreType.DMA((2, 2)),
            pltpu.SemaphoreType.DMA((2, 2)),
            pltpu.SemaphoreType.DMA((2, width // 512)),
            pltpu.SemaphoreType.DMA,
            pltpu.SemaphoreType.DMA((count // block,)),
            pltpu.SemaphoreType.DMA,
            pltpu.SemaphoreType.DMA((count // block,)),
        ],
        compiler_params=pltpu.CompilerParams(
            collective_id=0, has_side_effects=True, vmem_limit_bytes=56 * 1024 * 1024
        ),
        name="layer",
    )(
        in_gate.transpose(0, 2, 1),
        forget_gate.transpose(0, 2, 1),
        routes.T,
        route_weight.T,
        head_gain.reshape(1, -1),
        norm_gain.reshape(1, -1),
        queries,
        keys,
        values,
        out_gate,
        residual,
        w_out,
        shared_gate,
        shared_up,
        shared_down,
        w_gate,
        w_up,
        w_down,
    )


def solution(mesh):
    finer = Mesh(mesh.devices.reshape(4, 4, 4, mesh.shape["tp"]), SP_TP)
    return jax.shard_map(
        local,
        mesh=finer,
        in_specs=(
            P(SP_TP, None),
            P(SP, "tp"),
            P(SP, "tp"),
            P(SP, "tp"),
            P(SP, "tp"),
            P(None, SP, "tp"),
            P(None, SP, "tp"),
            P("tp"),
            P("tp", None),
            P(),
            P(),
            P(),
            P(),
            P(SP_TP, None, None),
            P(SP_TP, None, None),
            P(SP_TP, None, None),
            P(SP_TP, None),
            P(SP_TP, None),
        ),
        out_specs=P(SP_TP, None),
        check_vma=False,
    )
```
